256 devices in a mesh: grp: 2 (over y), ra: 16 (over z), cb: 4 (over x), dp: 2 (over core).
Axes of the slice: x: 4, y: 2, z: 16, core: 2. Of those that a mesh axis runs over, the one named last changes fastest.
The devices are a block of a 4x16x16 slice.
Arguments:
- tokens: bfloat16 [256, 2048], P(('grp', 'dp'), 'ra'), parts along dimension 0, may hold values from -62 to 62
- gain_first: float32 [2048], P('ra'), may hold values from 0.1 to 1.9
- up_first: bfloat16 [2048, 8192], P('ra', 'cb'), may hold values from -0.125 to 0.125
- down_first: bfloat16 [8192, 2048], P('cb', 'ra'), may hold values from -0.0625 to 0.0625
- gain_second: float32 [2048], P('ra'), may hold values from 0.1 to 1.9
- up_second: bfloat16 [2048, 8192], P('ra', 'cb'), may hold values from -0.125 to 0.125
- down_second: bfloat16 [8192, 2048], P('cb', 'ra'), may hold values from -0.0625 to 0.0625
- gain_last: float32 [2048], P('ra'), may hold values from 0.1 to 1.9
Outputs:
- normed: bfloat16 [256, 2048], P(('grp', 'dp'), 'ra'), parts along dimension 0
The draws below stay inside these ranges and needn't reach their ends.
There are 2 independent parts, one for each index of `grp`. The reference program is written for one: setup_inputs(seed, part) draws one part's arguments, and reference() takes and returns one part's arrays. A program takes and returns all parts, laid end to end along the dimension named above; an argument that names none is the same for every part. Nothing has to cross between parts.
All inputs are finite; a program needn't handle non-finite values.
Results may differ from the reference program's by a relative error of at most 0.0095.
Values may be sent and summed in bfloat16 or wider, within the bound.
No kernel may reach another device: no remote copies, remote signals or barrier semaphores. Data moves between devices by JAX's collectives and lax.ppermute only.
A program may use at most 64 MiB of HBM per device.

```python
import jax
import jax.numpy as jnp
from jax import lax

D = 2048
FF = 8192
TOKENS = 128


def draw_tokens(key, part):
    key_base = jax.random.fold_in(key, 11)
    key_cols = jax.random.fold_in(key, 12)
    key_rows = jax.random.fold_in(key, 13)
    position = jnp.arange(D, dtype=jnp.float32) / D
    columns = 10.0 ** (position - 0.5) * jnp.exp(jax.random.uniform(key_cols, (D,), jnp.float32, -0.7, 0.7))
    base = jnp.clip(jax.random.normal(key_base, (TOKENS, D), jnp.float32), -6.0, 6.0)
    rows = jnp.exp(jax.random.uniform(key_rows, (TOKENS, 1), jnp.float32, -1.15, 1.15))
    return jnp.clip(base * rows * columns, -62.0, 62.0).astype(jnp.bfloat16)


def steps_of(key, shape, shards, low, high):
    def one(axis_at, blocks):
        steps = jax.random.uniform(jax.random.fold_in(jax.random.fold_in(key, 6), axis_at), (blocks,), jnp.float32, low / len(shards), high / len(shards))
        return jnp.repeat(jnp.exp(steps), shape[axis_at] // blocks).reshape((-1,) + (1,) * (len(shape) - axis_at - 1))

    loudness = one(*shards[0])
    for cut in shards[1:]:
        loudness = loudness * one(*cut)
    return loudness


def normal_values(stream_key, dims, scale, bound, split=(), kind=jnp.bfloat16):
    result = scale * jax.random.normal(stream_key, dims, jnp.float32)
    if split:
        result = result * steps_of(stream_key, dims, split, -0.22, 0.18)
    return jnp.clip(result, -bound, bound).astype(kind)


def setup_inputs(seed: int = 0, part: int = 0) -> dict:
    arg_keys = jax.random.split(jax.random.key(seed), 9)
    part_keys = jax.random.split(jax.random.fold_in(arg_keys[8], part), 9)
    tokens = draw_tokens(jax.random.fold_in(jax.random.fold_in(arg_keys[8], part), 71), part)
    gain_first = jnp.clip(1.0 + 0.18 * jax.random.normal(arg_keys[1], (D,), jnp.float32), 0.1, 1.9)
    up_first = normal_values(arg_keys[2], (D, FF), D ** -0.5, 0.125, ((0, 16), (1, 4)))
    down_first = normal_values(arg_keys[3], (FF, D), FF ** -0.5, 0.0625, ((0, 4), (1, 16)))
    gain_second = jnp.clip(1.0 + 0.18 * jax.random.normal(arg_keys[4], (D,), jnp.float32), 0.1, 1.9)
    up_second = normal_values(arg_keys[5], (D, FF), D ** -0.5, 0.125, ((0, 16), (1, 4)))
    down_second = normal_values(arg_keys[6], (FF, D), FF ** -0.5, 0.0625, ((0, 4), (1, 16)))
    gain_last = jnp.clip(1.0 + 0.18 * jax.random.normal(arg_keys[7], (D,), jnp.float32), 0.1, 1.9)
    return dict(tokens=tokens, gain_first=gain_first, up_first=up_first, down_first=down_first, gain_second=gain_second, up_second=up_second, down_second=down_second, gain_last=gain_last)


EPS = 1e-06

def norm_inverse(h32):
    return lax.rsqrt(lax.optimization_barrier(jnp.mean(h32 * h32, axis=1, keepdims=True)) + EPS)

def mlp_branch(h32, gain, w_up, w_down):
    scaled = (h32 * gain).astype(jnp.bfloat16)
    pre = jnp.dot(scaled, w_up, preferred_element_type=jnp.float32) * norm_inverse(h32)
    hidden = jnp.square(jax.nn.relu(pre)).astype(jnp.bfloat16)
    return jnp.dot(hidden, w_down, preferred_element_type=jnp.float32)

def reference(tokens, gain_first, up_first, down_first, gain_second, up_second, down_second, gain_last):
    start32 = tokens.astype(jnp.float32)
    first = (0.5 * start32 + mlp_branch(start32, gain_first, up_first, down_first)).astype(jnp.bfloat16)
    first32 = first.astype(jnp.float32)
    second = (0.5 * first32 + mlp_branch(first32, gain_second, up_second, down_second)).astype(jnp.bfloat16)
    second32 = second.astype(jnp.float32)
    return (second32 * norm_inverse(second32) * gain_last).astype(jnp.bfloat16)
```

```python
import jax
import jax.numpy as jnp
from jax import lax
from jax.sharding import PartitionSpec as P

EPS = 1e-06
F32 = jnp.float32
BF16 = jnp.bfloat16


def exchange(pieces, axis):
    return lax.all_to_all(pieces, axis, split_axis=0, concat_axis=0, tiled=True)


def sent_to_all(shard, axis):
    return exchange(jnp.broadcast_to(shard, (lax.axis_size(axis), *shard.shape)), axis)


def local_squares(h32):
    return jnp.sum(h32 * h32, axis=1)


def packed_row(values):
    high = lax.reduce_precision(values, 8, 7)
    row = jnp.concatenate([high, values - high])[None, :]
    return jnp.pad(row, ((0, 7), (0, 0))).astype(BF16)


def mlp_branch(h32, gain, w_up, w_down):
    rows, lanes = h32.shape
    ra = lax.axis_size("ra")
    scaled = (h32 * gain).astype(BF16)
    partial_value = jnp.dot(scaled, w_up, preferred_element_type=F32).astype(BF16)
    pieces = jnp.moveaxis(partial_value.reshape(rows, ra, -1), 1, 0)
    shared = exchange(pieces, "ra").astype(F32).sum(axis=0)
    hidden_share = jnp.square(jax.nn.relu(shared)).astype(BF16)
    share = jnp.concatenate([hidden_share, packed_row(local_squares(h32))], axis=0)
    everyone = sent_to_all(share, "ra")
    hidden = jnp.moveaxis(everyone[:, :rows], 0, 1).reshape(rows, -1)
    squares = everyone[:, rows].astype(F32).sum(axis=0)
    mean_sq = (squares[:rows] + squares[rows:]) / (ra * lanes)
    down = jnp.dot(hidden, w_down, preferred_element_type=F32)
    return sent_to_all(down, "cb").sum(axis=0) / (mean_sq + EPS)[:, None]


def local(tokens, gain_first, up_first, down_first, gain_second, up_second, down_second, gain_last):
    start32 = tokens.astype(F32)
    first = (0.5 * start32 + mlp_branch(start32, gain_first, up_first, down_first)).astype(BF16)
    first32 = first.astype(F32)
    second = (0.5 * first32 + mlp_branch(first32, gain_second, up_second, down_second)).astype(BF16)
    second32 = second.astype(F32)
    squares = sent_to_all(local_squares(second32), "ra").sum(axis=0)
    inverse = lax.rsqrt(squares / (lax.axis_size("ra") * second.shape[1]) + EPS)
    return (second32 * inverse[:, None] * gain_last).astype(BF16)


def solution(mesh):
    return jax.shard_map(
        local,
        mesh=mesh,
        in_specs=(
            P(("grp", "dp"), "ra"),
            P("ra"),
            P("ra", "cb"),
            P("cb", "ra"),
            P("ra"),
            P("ra", "cb"),
            P("cb", "ra"),
            P("ra"),
        ),
        out_specs=P(("grp", "dp"), "ra"),
        check_vma=False,
    )
```

```python
import jax
import jax.numpy as jnp
from jax import lax
from jax.experimental import pallas as pl
from jax.experimental.pallas import tpu as pltpu
from jax.sharding import PartitionSpec as P

EPS = 1e-06
F32 = jnp.float32
BF16 = jnp.bfloat16
STAGGER_NS = 13000
STAGGER_CORE = 1
UP_COST = 2 << 20


def exchange(pieces, axis):
    return lax.all_to_all(pieces, axis, split_axis=0, concat_axis=0, tiled=True)


def sent_to_all(shard, axis):
    return exchange(jnp.broadcast_to(shard, (lax.axis_size(axis), *shard.shape)), axis)


def summed_over(value, axis):
    size = lax.axis_size(axis)
    total = value
    for step in range(1, size):
        total = total + lax.ppermute(value, axis, [(i, (i + step) % size) for i in range(size)])
    return total


def packed_row(h32):
    sums = jnp.sum(h32 * h32, axis=1)
    high = lax.reduce_precision(sums, 8, 7)
    row = jnp.stack([high, sums - high])
    return jnp.pad(row, ((0, 6), (0, h32.shape[1] - sums.shape[0]))).astype(BF16)


def write_pieces(scaled, up_ref, pieces_ref, piece):
    width = pieces_ref.shape[2]
    lanes = pl.ds(piece * width, width)
    pieces_ref[piece] = jnp.dot(scaled, up_ref[:, lanes], preferred_element_type=F32).astype(BF16)


def write_squares(h32, squares_ref):
    sums = jnp.sum(jnp.transpose(h32 * h32), axis=0, keepdims=True)
    rows = sums.shape[1]
    high = sums.astype(BF16).astype(F32)
    row = lax.broadcasted_iota(jnp.int32, (8, rows), 0)
    packed = jnp.where(row == 0, high, jnp.where(row == 1, sums - high, 0.0))
    squares_ref[:, :rows] = packed.astype(BF16)
    squares_ref[:, rows:] = jnp.zeros((8, squares_ref.shape[1] - rows), BF16)


def first_up_body(
    h_hbm, gain_hbm, up_hbm, pieces_hbm, h_ref, gain_ref, up_ref, pieces_ref, small_sems, in_sems, out_sems
):
    chunks = in_sems.shape[0]
    width = up_ref.shape[1] // chunks
    per_chunk = pieces_ref.shape[0] // chunks
    small = [
        pltpu.make_async_copy(h_hbm, h_ref, small_sems.at[0]),
        pltpu.make_async_copy(gain_hbm, gain_ref, small_sems.at[1]),
    ]
    arriving = [
        pltpu.make_async_copy(
            up_hbm.at[:, pl.ds(i * width, width)], up_ref.at[:, pl.ds(i * width, width)], in_sems.at[i]
        )
        for i in range(chunks)
    ]
    leaving = [
        pltpu.make_async_copy(
            pieces_ref.at[pl.ds(i * per_chunk, per_chunk)],
            pieces_hbm.at[pl.ds(i * per_chunk, per_chunk)],
            out_sems.at[i],
        )
        for i in range(chunks)
    ]
    for copy in small + arriving:
        copy.start()
    if STAGGER_NS:

        @pl.when(lax.axis_index("dp") == STAGGER_CORE)
        def _():
            pl.delay(STAGGER_NS)

    for copy in small:
        copy.wait()
    scaled = (h_ref[...].astype(F32) * gain_ref[...]).astype(BF16)
    for i in range(chunks):
        arriving[i].wait()
        for piece in range(i * per_chunk, (i + 1) * per_chunk):
            write_pieces(scaled, up_ref, pieces_ref, piece)
        leaving[i].start()
    for copy in leaving:
        copy.wait()


def up_body(h_ref, gain_ref, up_ref, pieces_ref, squares_ref):
    h32 = h_ref[...].astype(F32)
    scaled = (h32 * gain_ref[:1]).astype(BF16)
    for piece in range(pieces_ref.shape[0]):
        write_pieces(scaled, up_ref, pieces_ref, piece)
    write_squares(h32, squares_ref)


def up_shapes(h, w_up):
    ra = lax.axis_size("ra")
    return (
        jax.ShapeDtypeStruct((ra, h.shape[0], w_up.shape[1] // ra), BF16),
        jax.ShapeDtypeStruct((8, h.shape[1]), BF16),
    )


def up_costs(h, w_up):
    return pl.CostEstimate(
        flops=2 * h.size * w_up.shape[1], bytes_accessed=UP_COST, transcendentals=0
    )


def first_up(h, gain, w_up):
    chunks = 4
    pieces, _ = up_shapes(h, w_up)
    hbm = pl.BlockSpec(memory_space=pl.ANY)
    return pl.pallas_call(
        first_up_body,
        out_shape=pieces,
        in_specs=[hbm] * 3,
        out_specs=hbm,
        scratch_shapes=[
            pltpu.VMEM(h.shape, h.dtype),
            pltpu.VMEM(gain.shape, gain.dtype),
            pltpu.VMEM(w_up.shape, w_up.dtype),
            pltpu.VMEM(pieces.shape, pieces.dtype),
            pltpu.SemaphoreType.DMA((2,)),
            pltpu.SemaphoreType.DMA((chunks,)),
            pltpu.SemaphoreType.DMA((chunks,)),
        ],
        compiler_params=pltpu.CompilerParams(vmem_limit_bytes=66_000_000),
        cost_estimate=up_costs(h, w_up),
        name="first_up",
    )(h, gain, w_up)


def second_up(h, gain, w_up):
    return pl.pallas_call(
        up_body,
        out_shape=up_shapes(h, w_up),
        compiler_params=pltpu.CompilerParams(vmem_limit_bytes=8 * 1024 * 1024),
        cost_estimate=up_costs(h, w_up),
        name="second_up",
    )(h, gain, w_up)


def branch_of(pieces, packed, w_down, beside):
    ra, rows, _ = pieces.shape
    arrived, packed, beside = lax.optimization_barrier((exchange(pieces, "ra"), packed, beside))
    shared = arrived.astype(F32).sum(axis=0)
    hidden_share = jnp.square(jax.nn.relu(shared)).astype(BF16)
    everyone = sent_to_all(jnp.concatenate([hidden_share, packed], axis=0), "ra")
    hidden = jnp.moveaxis(everyone[:, :rows], 0, 1).reshape(rows, -1)
    squares = everyone[:, rows : rows + 2, :rows].astype(F32).sum(axis=(0, 1))
    mean_sq = squares / (ra * packed.shape[1])
    down = jnp.dot(hidden, w_down, preferred_element_type=F32)
    return summed_over(down, "cb") / (mean_sq + EPS)[:, None], beside


def local(tokens, gain_first, up_first, down_first, gain_second, up_second, down_second, gain_last):
    pieces = first_up(tokens, gain_first[None, :], up_first)
    pieces, tokens, gain_second, gain_last = lax.optimization_barrier(
        (pieces, tokens, gain_second, gain_last)
    )
    start = tokens.astype(F32)
    gains = lax.optimization_barrier(
        tuple(jnp.broadcast_to(gain, (8, *gain.shape)) for gain in (gain_second, gain_last))
    )
    branch, gains = branch_of(pieces, packed_row(start), down_first, gains)
    first = (0.5 * start + branch).astype(BF16)
    pieces, packed = second_up(first, gains[0], up_second)
    branch, gains = branch_of(pieces, packed, down_second, gains)
    second = (0.5 * first.astype(F32) + branch).astype(BF16)
    second32 = second.astype(F32)
    squares = sent_to_all(jnp.sum(second32 * second32, axis=1), "ra").sum(axis=0)
    inverse = lax.rsqrt(squares / (lax.axis_size("ra") * second.shape[1]) + EPS)
    return (second32 * inverse[:, None] * gains[1][0]).astype(BF16)


def solution(mesh):
    return jax.shard_map(
        local,
        mesh=mesh,
        in_specs=(
            P(("grp", "dp"), "ra"),
            P("ra"),
            P("ra", "cb"),
            P("cb", "ra"),
            P("ra"),
            P("ra", "cb"),
            P("cb", "ra"),
            P("ra"),
        ),
        out_specs=P(("grp", "dp"), "ra"),
        check_vma=False,
    )
```

```python
import jax
import jax.numpy as jnp
from jax import lax
from jax.experimental import pallas as pl
from jax.experimental.pallas import tpu as pltpu
from jax.sharding import PartitionSpec as P

EPS = 1e-06
F32 = jnp.float32
BF16 = jnp.bfloat16
STAGGER_NS = 13000
STAGGER_CORE = 1
LEAD_EIGHTHS = 6
SUM_TYPE = BF16
UP_COST = 2 << 20


def turned(size):
    lead = size * LEAD_EIGHTHS // 8
    return [(lead + i) % size for i in range(size)]


def exchange(pieces):
    order = turned(lax.axis_size("ra"))
    return lax.all_to_all(
        pieces, "ra", split_axis=0, concat_axis=0, tiled=True, axis_index_groups=[order]
    )


def sent_to_all(shard):
    return exchange(jnp.broadcast_to(shard, (lax.axis_size("ra"), *shard.shape)))


def summed_over(value, axis):
    size = lax.axis_size(axis)
    total = value
    sent = value.astype(SUM_TYPE)
    for step in range(1, size):
        pairs = [(i, (i + step) % size) for i in range(size)]
        total = total + lax.ppermute(sent, axis, pairs).astype(F32)
    return total


def packed_row(h32):
    sums = jnp.sum(h32 * h32, axis=1)
    high = lax.reduce_precision(sums, 8, 7)
    row = jnp.stack([high, sums - high])
    return jnp.pad(row, ((0, 6), (0, h32.shape[1] - sums.shape[0]))).astype(BF16)


def write_pieces(scaled, up_ref, pieces_ref, piece):
    width = pieces_ref.shape[2]
    lanes = pl.ds(piece * width, width)
    pieces_ref[turned(pieces_ref.shape[0]).index(piece)] = jnp.dot(scaled, up_ref[:, lanes], preferred_element_type=F32).astype(BF16)


def write_squares(h32, squares_ref):
    sums = jnp.sum(jnp.transpose(h32 * h32), axis=0, keepdims=True)
    rows = sums.shape[1]
    high = sums.astype(BF16).astype(F32)
    row = lax.broadcasted_iota(jnp.int32, (8, rows), 0)
    packed = jnp.where(row == 0, high, jnp.where(row == 1, sums - high, 0.0))
    squares_ref[:, :rows] = packed.astype(BF16)
    squares_ref[:, rows:] = jnp.zeros((8, squares_ref.shape[1] - rows), BF16)


def first_up_body(
    h_hbm, gain_hbm, up_hbm, pieces_hbm, h_ref, gain_ref, up_ref, pieces_ref, small_sems, in_sems, out_sems
):
    chunks = in_sems.shape[0]
    width = up_ref.shape[1] // chunks
    per_chunk = pieces_ref.shape[0] // chunks
    order = turned(pieces_ref.shape[0])
    small = [
        pltpu.make_async_copy(h_hbm, h_ref, small_sems.at[0]),
        pltpu.make_async_copy(gain_hbm, gain_ref, small_sems.at[1]),
    ]
    arriving = [
        pltpu.make_async_copy(
            up_hbm.at[:, pl.ds(i * width, width)], up_ref.at[:, pl.ds(i * width, width)], in_sems.at[i]
        )
        for i in range(chunks)
    ]
    leaving = [
        pltpu.make_async_copy(
            pieces_ref.at[pl.ds(i * per_chunk, per_chunk)],
            pieces_hbm.at[pl.ds(i * per_chunk, per_chunk)],
            out_sems.at[i],
        )
        for i in range(chunks)
    ]
    for copy in small + arriving:
        copy.start()
    if STAGGER_NS:

        @pl.when(lax.axis_index("dp") == STAGGER_CORE)
        def _():
            pl.delay(STAGGER_NS)

    for copy in small:
        copy.wait()
    scaled = (h_ref[...].astype(F32) * gain_ref[...]).astype(BF16)
    for i in range(chunks):
        arriving[i].wait()
        for piece in range(i * per_chunk, (i + 1) * per_chunk):
            write_pieces(scaled, up_ref, pieces_ref, piece)
        leaving[order.index(i * per_chunk) // per_chunk].start()
    for copy in leaving:
        copy.wait()


def up_body(h_ref, gain_ref, up_ref, pieces_ref, squares_ref):
    h32 = h_ref[...].astype(F32)
    scaled = (h32 * gain_ref[:1]).astype(BF16)
    for piece in range(pieces_ref.shape[0]):
        write_pieces(scaled, up_ref, pieces_ref, piece)
    write_squares(h32, squares_ref)


def up_shapes(h, w_up):
    ra = lax.axis_size("ra")
    return (
        jax.ShapeDtypeStruct((ra, h.shape[0], w_up.shape[1] // ra), BF16),
        jax.ShapeDtypeStruct((8, h.shape[1]), BF16),
    )


def up_costs(h, w_up):
    return pl.CostEstimate(
        flops=2 * h.size * w_up.shape[1], bytes_accessed=UP_COST, transcendentals=0
    )


def first_up(h, gain, w_up):
    chunks = 4
    pieces, _ = up_shapes(h, w_up)
    hbm = pl.BlockSpec(memory_space=pl.ANY)
    return pl.pallas_call(
        first_up_body,
        out_shape=pieces,
        in_specs=[hbm] * 3,
        out_specs=hbm,
        scratch_shapes=[
            pltpu.VMEM(h.shape, h.dtype),
            pltpu.VMEM(gain.shape, gain.dtype),
            pltpu.VMEM(w_up.shape, w_up.dtype),
            pltpu.VMEM(pieces.shape, pieces.dtype),
            pltpu.SemaphoreType.DMA((2,)),
            pltpu.SemaphoreType.DMA((chunks,)),
            pltpu.SemaphoreType.DMA((chunks,)),
        ],
        compiler_params=pltpu.CompilerParams(vmem_limit_bytes=66_000_000),
        cost_estimate=up_costs(h, w_up),
        name="first_up",
    )(h, gain, w_up)


def second_up(h, gain, w_up):
    return pl.pallas_call(
        up_body,
        out_shape=up_shapes(h, w_up),
        compiler_params=pltpu.CompilerParams(vmem_limit_bytes=8 * 1024 * 1024),
        cost_estimate=up_costs(h, w_up),
        name="second_up",
    )(h, gain, w_up)


def down_body(everyone_ref, down_ref, out_ref):
    rows, lanes = out_ref.shape[0], everyone_ref.shape[2]
    order = turned(everyone_ref.shape[0])
    total = jnp.zeros(out_ref.shape, F32)
    for block in range(0, len(order), 2):
        pair = [everyone_ref[order.index(block + k), :rows, :] for k in range(2)]
        weights = down_ref[pl.ds(block * lanes, 2 * lanes), :]
        total = total + jnp.dot(
            jnp.concatenate(pair, axis=1), weights, preferred_element_type=F32
        )
    out_ref[...] = total


def down_sums(everyone, w_down, rows):
    return pl.pallas_call(
        down_body,
        out_shape=jax.ShapeDtypeStruct((rows, w_down.shape[1]), F32),
        compiler_params=pltpu.CompilerParams(vmem_limit_bytes=8 * 1024 * 1024),
        cost_estimate=pl.CostEstimate(
            flops=2 * rows * w_down.size, bytes_accessed=UP_COST, transcendentals=0
        ),
        name="down_sums",
    )(everyone, w_down)


def branch_of(pieces, packed, w_down, beside):
    ra, rows, _ = pieces.shape
    arrived, packed, beside = lax.optimization_barrier((exchange(pieces), packed, beside))
    shared = arrived.astype(F32).sum(axis=0)
    hidden_share = jnp.square(jax.nn.relu(shared)).astype(BF16)
    everyone = sent_to_all(jnp.concatenate([hidden_share, packed], axis=0))
    squares = everyone[:, rows : rows + 2, :rows].astype(F32).sum(axis=(0, 1))
    mean_sq = squares / (ra * packed.shape[1])
    down = down_sums(everyone, w_down, rows)
    return summed_over(down, "cb") / (mean_sq + EPS)[:, None], beside


def local(tokens, gain_first, up_first, down_first, gain_second, up_second, down_second, gain_last):
    pieces = first_up(tokens, gain_first[None, :], up_first)
    pieces, tokens, gain_second, gain_last = lax.optimization_barrier(
        (pieces, tokens, gain_second, gain_last)
    )
    start = tokens.astype(F32)
    gains = lax.optimization_barrier(
        tuple(jnp.broadcast_to(gain, (*tokens.shape[:1], *gain.shape)) for gain in (gain_second, gain_last))
    )
    branch, gains = branch_of(pieces, packed_row(start), down_first, gains)
    first = (0.5 * start + branch).astype(BF16)
    pieces, packed = second_up(first, gains[0], up_second)
    branch, gains = branch_of(pieces, packed, down_second, gains)
    second = (0.5 * first.astype(F32) + branch).astype(BF16)
    second32 = second.astype(F32)
    squares = sent_to_all(jnp.sum(second32 * second32, axis=1)).sum(axis=0)
    inverse = lax.rsqrt(squares / (lax.axis_size("ra") * second.shape[1]) + EPS)
    return (second32 * inverse[:, None] * gains[1]).astype(BF16)


def solution(mesh):
    return jax.shard_map(
        local,
        mesh=mesh,
        in_specs=(
            P(("grp", "dp"), "ra"),
            P("ra"),
            P("ra", "cb"),
            P("cb", "ra"),
            P("ra"),
            P("ra", "cb"),
            P("cb", "ra"),
            P("ra"),
        ),
        out_specs=P(("grp", "dp"), "ra"),
        check_vma=False,
    )
```

```python
import jax
import jax.numpy as jnp
from jax import lax
from jax.experimental import pallas as pl
from jax.experimental.pallas import tpu as pltpu
from jax.sharding import PartitionSpec as P

EPS = 1e-06
F32 = jnp.float32
BF16 = jnp.bfloat16
STAGGER_NS = 12800
STAGGER_CORE = 1
LEAD_EIGHTHS = 7
LAST_LEAD_EIGHTHS = 4
SUM_TYPE = BF16
UP_COST = 2 << 20
PAD = 8
CHUNKS = 2


def member_order(size, eighths=None):
    lead = size * (LEAD_EIGHTHS if eighths is None else eighths) // 8
    return [(lead + i) % size for i in range(size)]


def exchange(pieces, eighths=None):
    order = member_order(lax.axis_size("ra"), eighths)
    return lax.all_to_all(
        pieces, "ra", split_axis=0, concat_axis=0, tiled=True, axis_index_groups=[order]
    )


def sent_to_all(shard, eighths=None):
    return exchange(jnp.broadcast_to(shard, (lax.axis_size("ra"), *shard.shape)), eighths)


def summed_over(value, axis):
    size = lax.axis_size(axis)
    total = value
    sent = value.astype(SUM_TYPE)
    for step in range(1, size):
        pairs = [(i, (i + step) % size) for i in range(size)]
        total = total + lax.ppermute(sent, axis, pairs).astype(F32)
    return total


def write_piece(scaled, packed, up_ref, pieces_ref, piece):
    width = pieces_ref.shape[2]
    lanes = pl.ds(piece * width, width)
    sums = jnp.dot(scaled, up_ref[:, lanes], preferred_element_type=F32)
    place = member_order(pieces_ref.shape[0]).index(piece)
    pieces_ref[place, : scaled.shape[0], :] = sums.astype(BF16)
    pieces_ref[place, scaled.shape[0] :, :] = packed


def squares_row(h32):
    lanes = h32.shape[1]
    square = h32 * h32
    sums = jnp.sum(jnp.transpose(square), axis=0, keepdims=True)
    high = sums.astype(BF16).astype(F32)
    row = lax.broadcasted_iota(jnp.int32, (PAD, sums.shape[1]), 0)
    packed = jnp.where(row == 0, high, jnp.where(row == 1, sums - high, 0.0))
    rest = jnp.zeros((PAD, lanes - sums.shape[1]), F32)
    return jnp.concatenate([packed, rest], axis=1).astype(BF16)


def first_up_body(
    h_hbm, gain_hbm, up_hbm, pieces_hbm, h_ref, gain_ref, up_ref, pieces_ref, small_sems, in_sems, out_sems
):
    chunks = in_sems.shape[0]
    width = up_ref.shape[1] // chunks
    per_chunk = pieces_ref.shape[0] // chunks
    order = member_order(pieces_ref.shape[0])
    small = [
        pltpu.make_async_copy(h_hbm, h_ref, small_sems.at[0]),
        pltpu.make_async_copy(gain_hbm, gain_ref, small_sems.at[1]),
    ]
    arriving = [
        pltpu.make_async_copy(
            up_hbm.at[:, pl.ds(i * width, width)], up_ref.at[:, pl.ds(i * width, width)], in_sems.at[i]
        )
        for i in range(chunks)
    ]
    leaving = [
        pltpu.make_async_copy(
            pieces_ref.at[order.index(piece)], pieces_hbm.at[order.index(piece)], out_sems.at[piece]
        )
        for piece in range(len(order))
    ]
    for copy in small + arriving:
        copy.start()
    if STAGGER_NS:

        @pl.when(lax.axis_index("dp") == STAGGER_CORE)
        def _():
            pl.delay(STAGGER_NS)

    for copy in small:
        copy.wait()
    h32 = h_ref[...].astype(F32)
    scaled = (h32 * gain_ref[...]).astype(BF16)
    packed = squares_row(h32)
    for i in range(chunks):
        arriving[i].wait()
        for piece in range(i * per_chunk, (i + 1) * per_chunk):
            write_piece(scaled, packed, up_ref, pieces_ref, piece)
            leaving[piece].start()
    for copy in leaving:
        copy.wait()


def up_body(h_ref, gain_ref, up_ref, pieces_ref):
    h32 = h_ref[...].astype(F32)
    scaled = (h32 * gain_ref[:1]).astype(BF16)
    packed = squares_row(h32)
    for piece in range(pieces_ref.shape[0]):
        write_piece(scaled, packed, up_ref, pieces_ref, piece)


def up_shape(h, w_up):
    ra = lax.axis_size("ra")
    return jax.ShapeDtypeStruct((ra, h.shape[0] + PAD, w_up.shape[1] // ra), BF16)


def up_costs(h, w_up):
    return pl.CostEstimate(
        flops=2 * h.size * w_up.shape[1], bytes_accessed=UP_COST, transcendentals=0
    )


def first_up(h, gain, w_up):
    chunks = CHUNKS
    pieces = up_shape(h, w_up)
    hbm = pl.BlockSpec(memory_space=pl.ANY)
    return pl.pallas_call(
        first_up_body,
        out_shape=pieces,
        in_specs=[hbm] * 3,
        out_specs=hbm,
        scratch_shapes=[
            pltpu.VMEM(h.shape, h.dtype),
            pltpu.VMEM(gain.shape, gain.dtype),
            pltpu.VMEM(w_up.shape, w_up.dtype),
            pltpu.VMEM(pieces.shape, pieces.dtype),
            pltpu.SemaphoreType.DMA((2,)),
            pltpu.SemaphoreType.DMA((chunks,)),
            pltpu.SemaphoreType.DMA(pieces.shape[:1]),
        ],
        compiler_params=pltpu.CompilerParams(vmem_limit_bytes=66_000_000),
        cost_estimate=up_costs(h, w_up),
        name="first_up",
    )(h, gain, w_up)


def second_up(h, gain, w_up):
    return pl.pallas_call(
        up_body,
        out_shape=up_shape(h, w_up),
        compiler_params=pltpu.CompilerParams(vmem_limit_bytes=8 * 1024 * 1024),
        cost_estimate=up_costs(h, w_up),
        name="second_up",
    )(h, gain, w_up)


def down_body(everyone_ref, down_ref, out_ref):
    rows, lanes = out_ref.shape[0], everyone_ref.shape[2]
    order = member_order(everyone_ref.shape[0])
    total = jnp.zeros(out_ref.shape, F32)
    for block in range(0, len(order), 2):
        pair = [everyone_ref[order.index(block + k), :rows, :] for k in range(2)]
        weights = down_ref[pl.ds(block * lanes, 2 * lanes), :]
        total = total + jnp.dot(
            jnp.concatenate(pair, axis=1), weights, preferred_element_type=F32
        )
    out_ref[...] = total


def down_sums(everyone, w_down, rows):
    return pl.pallas_call(
        down_body,
        out_shape=jax.ShapeDtypeStruct((rows, w_down.shape[1]), F32),
        compiler_params=pltpu.CompilerParams(vmem_limit_bytes=8 * 1024 * 1024),
        cost_estimate=pl.CostEstimate(
            flops=2 * rows * w_down.size, bytes_accessed=UP_COST, transcendentals=0
        ),
        name="down_sums",
    )(everyone, w_down)


def branch_of(pieces, w_down, beside):
    ra, rows, lanes = pieces.shape
    rows -= PAD
    arrived, beside = lax.optimization_barrier((exchange(pieces), beside))
    shared = arrived[:, :rows].astype(F32).sum(axis=0)
    hidden_share = jnp.square(jax.nn.relu(shared)).astype(BF16)
    squares = arrived[:, rows : rows + 2, :rows].astype(F32).sum(axis=(0, 1))
    hidden_share, squares = lax.optimization_barrier((hidden_share, squares))
    everyone = sent_to_all(hidden_share)
    mean_sq = squares / (ra * w_down.shape[1])
    down = down_sums(everyone, w_down, rows)
    return summed_over(down, "cb") / (mean_sq + EPS)[:, None], beside


def local(tokens, gain_first, up_first, down_first, gain_second, up_second, down_second, gain_last):
    pieces = first_up(tokens, gain_first[None, :], up_first)
    pieces, tokens, gain_second, gain_last = lax.optimization_barrier(
        (pieces, tokens, gain_second, gain_last)
    )
    start = tokens.astype(F32)
    gains = lax.optimization_barrier(
        tuple(jnp.broadcast_to(gain, (*tokens.shape[:1], *gain.shape)) for gain in (gain_second, gain_last))
    )
    branch, gains = branch_of(pieces, down_first, gains)
    first = (0.5 * start + branch).astype(BF16)
    pieces = second_up(first, gains[0], up_second)
    branch, gains = branch_of(pieces, down_second, gains)
    second = (0.5 * first.astype(F32) + branch).astype(BF16)
    second32 = second.astype(F32)
    squares = sent_to_all(jnp.sum(second32 * second32, axis=1), LAST_LEAD_EIGHTHS).sum(axis=0)
    inverse = lax.rsqrt(squares / (lax.axis_size("ra") * second.shape[1]) + EPS)
    return (second32 * inverse[:, None] * gains[1]).astype(BF16)


def solution(mesh):
    return jax.shard_map(
        local,
        mesh=mesh,
        in_specs=(
            P(("grp", "dp"), "ra"),
            P("ra"),
            P("ra", "cb"),
            P("cb", "ra"),
            P("ra"),
            P("ra", "cb"),
            P("cb", "ra"),
            P("ra"),
        ),
        out_specs=P(("grp", "dp"), "ra"),
        check_vma=False,
    )
```

```python
import jax
import jax.numpy as jnp
from jax import lax
from jax.experimental import pallas as pl
from jax.experimental.pallas import tpu as pltpu
from jax.sharding import PartitionSpec as P

EPS = 1e-06
F32 = jnp.float32
BF16 = jnp.bfloat16
STAGGER_NS = 12700
STAGGER_CORE = 1
LEAD_EIGHTHS = 7
LAST_LEAD_EIGHTHS = 4
SUM_TYPE = BF16
UP_COST = 2 << 20
PAD = 8
CHUNKS = 2


def member_order(size, eighths=None):
    lead = size * (LEAD_EIGHTHS if eighths is None else eighths) // 8
    return [(lead + i) % size for i in range(size)]


def exchange(pieces, eighths=None):
    order = member_order(lax.axis_size("ra"), eighths)
    return lax.all_to_all(
        pieces, "ra", split_axis=0, concat_axis=0, tiled=True, axis_index_groups=[order]
    )


def sent_to_all(shard, eighths=None):
    return exchange(jnp.broadcast_to(shard, (lax.axis_size("ra"), *shard.shape)), eighths)


def summed_over(value, axis):
    size = lax.axis_size(axis)
    total = value
    sent = value.astype(SUM_TYPE)
    for step in range(1, size):
        pairs = [(i, i ^ step) for i in range(size)]
        total = total + lax.ppermute(sent, axis, pairs).astype(F32)
    return total


def write_piece(scaled, packed, up_ref, pieces_ref, piece):
    width = pieces_ref.shape[2]
    lanes = pl.ds(piece * width, width)
    sums = jnp.dot(scaled, up_ref[:, lanes], preferred_element_type=F32)
    place = member_order(pieces_ref.shape[0]).index(piece)
    pieces_ref[place, : scaled.shape[0], :] = sums.astype(BF16)
    pieces_ref[place, scaled.shape[0] :, :] = packed


def squares_row(h32):
    lanes = h32.shape[1]
    square = h32 * h32
    sums = jnp.sum(jnp.transpose(square), axis=0, keepdims=True)
    high = sums.astype(BF16).astype(F32)
    row = lax.broadcasted_iota(jnp.int32, (PAD, sums.shape[1]), 0)
    packed = jnp.where(row == 0, high, jnp.where(row == 1, sums - high, 0.0))
    rest = jnp.zeros((PAD, lanes - sums.shape[1]), F32)
    return jnp.concatenate([packed, rest], axis=1).astype(BF16)


def first_up_body(
    h_hbm, gain_hbm, up_hbm, pieces_hbm, h_ref, gain_ref, up_ref, pieces_ref, small_sems, in_sems, out_sems
):
    chunks = in_sems.shape[0]
    width = up_ref.shape[1] // chunks
    per_chunk = pieces_ref.shape[0] // chunks
    order = member_order(pieces_ref.shape[0])
    small = [
        pltpu.make_async_copy(h_hbm, h_ref, small_sems.at[0]),
        pltpu.make_async_copy(gain_hbm, gain_ref, small_sems.at[1]),
    ]
    arriving = [
        pltpu.make_async_copy(
            up_hbm.at[:, pl.ds(i * width, width)], up_ref.at[:, pl.ds(i * width, width)], in_sems.at[i]
        )
        for i in range(chunks)
    ]
    leaving = [
        pltpu.make_async_copy(
            pieces_ref.at[order.index(piece)], pieces_hbm.at[order.index(piece)], out_sems.at[piece]
        )
        for piece in range(len(order))
    ]
    for copy in small + arriving:
        copy.start()
    if STAGGER_NS:

        @pl.when(lax.axis_index("dp") == STAGGER_CORE)
        def _():
            pl.delay(STAGGER_NS)

    for copy in small:
        copy.wait()
    h32 = h_ref[...].astype(F32)
    scaled = (h32 * gain_ref[...]).astype(BF16)
    packed = squares_row(h32)
    for i in range(chunks):
        arriving[i].wait()
        for piece in range(i * per_chunk, (i + 1) * per_chunk):
            write_piece(scaled, packed, up_ref, pieces_ref, piece)
            leaving[piece].start()
    for copy in leaving:
        copy.wait()


def up_body(h_ref, gain_ref, up_ref, pieces_ref):
    h32 = h_ref[...].astype(F32)
    scaled = (h32 * gain_ref[:1]).astype(BF16)
    packed = squares_row(h32)
    for piece in range(pieces_ref.shape[0]):
        write_piece(scaled, packed, up_ref, pieces_ref, piece)


def up_shape(h, w_up):
    ra = lax.axis_size("ra")
    return jax.ShapeDtypeStruct((ra, h.shape[0] + PAD, w_up.shape[1] // ra), BF16)


def up_costs(h, w_up):
    return pl.CostEstimate(
        flops=2 * h.size * w_up.shape[1], bytes_accessed=UP_COST, transcendentals=0
    )


def first_up(h, gain, w_up):
    chunks = CHUNKS
    pieces = up_shape(h, w_up)
    hbm = pl.BlockSpec(memory_space=pl.ANY)
    return pl.pallas_call(
        first_up_body,
        out_shape=pieces,
        in_specs=[hbm] * 3,
        out_specs=hbm,
        scratch_shapes=[
            pltpu.VMEM(h.shape, h.dtype),
            pltpu.VMEM(gain.shape, gain.dtype),
            pltpu.VMEM(w_up.shape, w_up.dtype),
            pltpu.VMEM(pieces.shape, pieces.dtype),
            pltpu.SemaphoreType.DMA((2,)),
            pltpu.SemaphoreType.DMA((chunks,)),
            pltpu.SemaphoreType.DMA(pieces.shape[:1]),
        ],
        compiler_params=pltpu.CompilerParams(vmem_limit_bytes=66_000_000),
        cost_estimate=up_costs(h, w_up),
        name="first_up",
    )(h, gain, w_up)


def second_up(h, gain, w_up):
    return pl.pallas_call(
        up_body,
        out_shape=up_shape(h, w_up),
        compiler_params=pltpu.CompilerParams(vmem_limit_bytes=8 * 1024 * 1024),
        cost_estimate=up_costs(h, w_up),
        name="second_up",
    )(h, gain, w_up)


def down_body(everyone_ref, down_ref, out_ref):
    rows, lanes = out_ref.shape[0], everyone_ref.shape[2]
    order = member_order(everyone_ref.shape[0])
    total = jnp.zeros(out_ref.shape, F32)
    for block in range(0, len(order), 2):
        pair = [everyone_ref[order.index(block + k), :rows, :] for k in range(2)]
        weights = down_ref[pl.ds(block * lanes, 2 * lanes), :]
        total = total + jnp.dot(
            jnp.concatenate(pair, axis=1), weights, preferred_element_type=F32
        )
    out_ref[...] = total


def down_sums(everyone, w_down, rows):
    return pl.pallas_call(
        down_body,
        out_shape=jax.ShapeDtypeStruct((rows, w_down.shape[1]), F32),
        compiler_params=pltpu.CompilerParams(vmem_limit_bytes=8 * 1024 * 1024),
        cost_estimate=pl.CostEstimate(
            flops=2 * rows * w_down.size, bytes_accessed=UP_COST, transcendentals=0
        ),
        name="down_sums",
    )(everyone, w_down)


def branch_of(pieces, w_down, beside):
    ra, rows, lanes = pieces.shape
    rows -= PAD
    arrived, beside = lax.optimization_barrier((exchange(pieces), beside))
    shared = arrived[:, :rows].astype(F32).sum(axis=0)
    hidden_share = jnp.square(jax.nn.relu(shared)).astype(BF16)
    squares = arrived[:, rows : rows + 2, :rows].astype(F32).sum(axis=(0, 1))
    hidden_share, squares = lax.optimization_barrier((hidden_share, squares))
    everyone = sent_to_all(hidden_share)
    mean_sq = squares / (ra * w_down.shape[1])
    down = down_sums(everyone, w_down, rows)
    return summed_over(down, "cb") / (mean_sq + EPS)[:, None], beside


def local(tokens, gain_first, up_first, down_first, gain_second, up_second, down_second, gain_last):
    pieces = first_up(tokens, gain_first[None, :], up_first)
    pieces, tokens, gain_second, gain_last = lax.optimization_barrier(
        (pieces, tokens, gain_second, gain_last)
    )
    start = tokens.astype(F32)
    gains = lax.optimization_barrier(
        tuple(jnp.broadcast_to(gain, (*tokens.shape[:1], *gain.shape)) for gain in (gain_second, gain_last))
    )
    branch, gains = branch_of(pieces, down_first, gains)
    first = (0.5 * start + branch).astype(BF16)
    pieces = second_up(first, gains[0], up_second)
    branch, gains = branch_of(pieces, down_second, gains)
    second = (0.5 * first.astype(F32) + branch).astype(BF16)
    second32 = second.astype(F32)
    squares = sent_to_all(jnp.sum(second32 * second32, axis=1), LAST_LEAD_EIGHTHS).sum(axis=0)
    inverse = lax.rsqrt(squares / (lax.axis_size("ra") * second.shape[1]) + EPS)
    return (second32 * inverse[:, None] * gains[1]).astype(BF16)


def solution(mesh):
    return jax.shard_map(
        local,
        mesh=mesh,
        in_specs=(
            P(("grp", "dp"), "ra"),
            P("ra"),
            P("ra", "cb"),
            P("cb", "ra"),
            P("ra"),
            P("ra", "cb"),
            P("cb", "ra"),
            P("ra"),
        ),
        out_specs=P(("grp", "dp"), "ra"),
        check_vma=False,
    )
```

```python
import jax
import jax.numpy as jnp
from jax import lax
from jax.experimental import pallas as pl
from jax.experimental.pallas import tpu as pltpu
from jax.sharding import PartitionSpec as P

EPS = 1e-06
F32 = jnp.float32
BF16 = jnp.bfloat16
STAGGER_NS = 13200
STAGGER_CORE = 1
LEAD_EIGHTHS = 7
LAST_LEAD_EIGHTHS = 4
UP_COST = 2 << 20
PAD = 8
CHUNKS = 2


def member_order(size, eighths=None):
    lead = size * (LEAD_EIGHTHS if eighths is None else eighths) // 8
    return [(lead + i) % size for i in range(size)]


def exchange(pieces, eighths=None):
    order = member_order(lax.axis_size("ra"), eighths)
    return lax.all_to_all(
        pieces, "ra", split_axis=0, concat_axis=0, tiled=True, axis_index_groups=[order]
    )


def sent_to_all(shard, eighths=None):
    return exchange(jnp.broadcast_to(shard, (lax.axis_size("ra"), *shard.shape)), eighths)


def summed_over(total, sent, axis):
    size = lax.axis_size(axis)
    for step in range(1, size):
        pairs = [(i, i ^ step) for i in range(size)]
        total = total + lax.ppermute(sent, axis, pairs).astype(F32)
    return total


def write_piece(scaled, packed, up_ref, pieces_ref, piece):
    width = pieces_ref.shape[2]
    lanes = pl.ds(piece * width, width)
    sums = jnp.dot(scaled, up_ref[:, lanes], preferred_element_type=F32)
    place = member_order(pieces_ref.shape[0]).index(piece)
    pieces_ref[place, : scaled.shape[0], :] = sums.astype(BF16)
    pieces_ref[place, scaled.shape[0] :, :] = packed


def squares_row(h32):
    lanes = h32.shape[1]
    square = h32 * h32
    sums = jnp.sum(jnp.transpose(square), axis=0, keepdims=True)
    high = sums.astype(BF16).astype(F32)
    row = lax.broadcasted_iota(jnp.int32, (PAD, sums.shape[1]), 0)
    packed = jnp.where(row == 0, high, jnp.where(row == 1, sums - high, 0.0))
    rest = jnp.zeros((PAD, lanes - sums.shape[1]), F32)
    return jnp.concatenate([packed, rest], axis=1).astype(BF16)


def first_up_body(
    h_hbm, gain_hbm, up_hbm, pieces_hbm, h_ref, gain_ref, up_ref, pieces_ref, small_sems, in_sems, out_sems
):
    chunks = in_sems.shape[0]
    width = up_ref.shape[1] // chunks
    per_chunk = pieces_ref.shape[0] // chunks
    order = member_order(pieces_ref.shape[0])
    small = [
        pltpu.make_async_copy(h_hbm, h_ref, small_sems.at[0]),
        pltpu.make_async_copy(gain_hbm, gain_ref, small_sems.at[1]),
    ]
    arriving = [
        pltpu.make_async_copy(
            up_hbm.at[:, pl.ds(i * width, width)], up_ref.at[:, pl.ds(i * width, width)], in_sems.at[i]
        )
        for i in range(chunks)
    ]
    leaving = [
        pltpu.make_async_copy(
            pieces_ref.at[order.index(piece)], pieces_hbm.at[order.index(piece)], out_sems.at[piece]
        )
        for piece in range(len(order))
    ]
    for copy in small + arriving:
        copy.start()
    if STAGGER_NS:

        @pl.when(lax.axis_index("dp") == STAGGER_CORE)
        def _():
            pl.delay(STAGGER_NS)

    for copy in small:
        copy.wait()
    h32 = h_ref[...].astype(F32)
    scaled = (h32 * gain_ref[...]).astype(BF16)
    packed = squares_row(h32)
    for i in range(chunks):
        arriving[i].wait()
        for piece in range(i * per_chunk, (i + 1) * per_chunk):
            write_piece(scaled, packed, up_ref, pieces_ref, piece)
            leaving[piece].start()
    for copy in leaving:
        copy.wait()


def up_body(h_ref, gain_ref, up_ref, pieces_ref):
    h32 = h_ref[...].astype(F32)
    scaled = (h32 * gain_ref[:1]).astype(BF16)
    packed = squares_row(h32)
    for piece in range(pieces_ref.shape[0]):
        write_piece(scaled, packed, up_ref, pieces_ref, piece)


def up_shape(h, w_up):
    ra = lax.axis_size("ra")
    return jax.ShapeDtypeStruct((ra, h.shape[0] + PAD, w_up.shape[1] // ra), BF16)


def up_costs(h, w_up):
    return pl.CostEstimate(
        flops=2 * h.size * w_up.shape[1], bytes_accessed=UP_COST, transcendentals=0
    )


def first_up(h, gain, w_up):
    chunks = CHUNKS
    pieces = up_shape(h, w_up)
    hbm = pl.BlockSpec(memory_space=pl.ANY)
    return pl.pallas_call(
        first_up_body,
        out_shape=pieces,
        in_specs=[hbm] * 3,
        out_specs=hbm,
        scratch_shapes=[
            pltpu.VMEM(h.shape, h.dtype),
            pltpu.VMEM(gain.shape, gain.dtype),
            pltpu.VMEM(w_up.shape, w_up.dtype),
            pltpu.VMEM(pieces.shape, pieces.dtype),
            pltpu.SemaphoreType.DMA((2,)),
            pltpu.SemaphoreType.DMA((chunks,)),
            pltpu.SemaphoreType.DMA(pieces.shape[:1]),
        ],
        compiler_params=pltpu.CompilerParams(vmem_limit_bytes=66_000_000),
        cost_estimate=up_costs(h, w_up),
        name="first_up",
    )(h, gain, w_up)


def second_up(h, gain, w_up):
    return pl.pallas_call(
        up_body,
        out_shape=up_shape(h, w_up),
        compiler_params=pltpu.CompilerParams(vmem_limit_bytes=8 * 1024 * 1024),
        cost_estimate=up_costs(h, w_up),
        name="second_up",
    )(h, gain, w_up)


def down_body(everyone_ref, down_ref, out_ref, sent_ref):
    rows, lanes = out_ref.shape[0], everyone_ref.shape[2]
    order = member_order(everyone_ref.shape[0])
    total = jnp.zeros(out_ref.shape, F32)
    for block in range(0, len(order), 2):
        pair = [everyone_ref[order.index(block + k), :rows, :] for k in range(2)]
        weights = down_ref[pl.ds(block * lanes, 2 * lanes), :]
        total = total + jnp.dot(
            jnp.concatenate(pair, axis=1), weights, preferred_element_type=F32
        )
    out_ref[...] = total
    sent_ref[...] = total.astype(BF16)


def down_sums(everyone, w_down, rows):
    return pl.pallas_call(
        down_body,
        out_shape=[jax.ShapeDtypeStruct((rows, w_down.shape[1]), kind) for kind in (F32, BF16)],
        compiler_params=pltpu.CompilerParams(vmem_limit_bytes=8 * 1024 * 1024),
        cost_estimate=pl.CostEstimate(
            flops=2 * rows * w_down.size, bytes_accessed=UP_COST, transcendentals=0
        ),
        name="down_sums",
    )(everyone, w_down)


def branch_of(pieces, w_down, beside):
    ra, rows, lanes = pieces.shape
    rows -= PAD
    arrived, beside = lax.optimization_barrier((exchange(pieces), beside))
    shared = arrived[:, :rows].astype(F32).sum(axis=0)
    hidden_share = jnp.square(jax.nn.relu(shared)).astype(BF16)
    squares = arrived[:, rows : rows + 2, :rows].astype(F32).sum(axis=(0, 1))
    hidden_share, squares = lax.optimization_barrier((hidden_share, squares))
    everyone = sent_to_all(hidden_share)
    mean_sq = squares / (ra * w_down.shape[1])
    return summed_over(*down_sums(everyone, w_down, rows), "cb") / (mean_sq + EPS)[:, None], beside


def local(tokens, gain_first, up_first, down_first, gain_second, up_second, down_second, gain_last):
    pieces = first_up(tokens, gain_first[None, :], up_first)
    pieces, tokens, gain_second, gain_last = lax.optimization_barrier(
        (pieces, tokens, gain_second, gain_last)
    )
    start = tokens.astype(F32)
    gains = lax.optimization_barrier(
        tuple(jnp.broadcast_to(gain, (*tokens.shape[:1], *gain.shape)) for gain in (gain_second, gain_last))
    )
    branch, gains = branch_of(pieces, down_first, gains)
    first = (0.5 * start + branch).astype(BF16)
    pieces = second_up(first, gains[0], up_second)
    branch, gains = branch_of(pieces, down_second, gains)
    second = (0.5 * first.astype(F32) + branch).astype(BF16)
    second32 = second.astype(F32)
    squares = sent_to_all(jnp.sum(second32 * second32, axis=1), LAST_LEAD_EIGHTHS).sum(axis=0)
    inverse = lax.rsqrt(squares / (lax.axis_size("ra") * second.shape[1]) + EPS)
    return (second32 * inverse[:, None] * gains[1]).astype(BF16)


def solution(mesh):
    return jax.shard_map(
        local,
        mesh=mesh,
        in_specs=(
            P(("grp", "dp"), "ra"),
            P("ra"),
            P("ra", "cb"),
            P("cb", "ra"),
            P("ra"),
            P("ra", "cb"),
            P("cb", "ra"),
            P("ra"),
        ),
        out_specs=P(("grp", "dp"), "ra"),
        check_vma=False,
    )
```

```python
import jax
import jax.numpy as jnp
from jax import lax
from jax.experimental import pallas as pl
from jax.experimental.pallas import tpu as pltpu
from jax.sharding import PartitionSpec as P

EPS = 1e-06
F32 = jnp.float32
BF16 = jnp.bfloat16
STAGGER_NS = 13300
STAGGER_CORE = 1
LEAD_EIGHTHS = 7
LAST_LEAD_EIGHTHS = 4
SUM_TYPE = BF16
UP_COST = 2 << 20
PAD = 8
CHUNKS = 2


def member_order(size, eighths=None):
    lead = size * (LEAD_EIGHTHS if eighths is None else eighths) // 8
    return [(lead + i) % size for i in range(size)]


def exchange(pieces, eighths=None):
    order = member_order(lax.axis_size("ra"), eighths)
    return lax.all_to_all(
        pieces, "ra", split_axis=0, concat_axis=0, tiled=True, axis_index_groups=[order]
    )


def sent_to_all(shard, eighths=None):
    return exchange(jnp.broadcast_to(shard, (lax.axis_size("ra"), *shard.shape)), eighths)


def summed_over(value, axis):
    size = lax.axis_size(axis)
    total = value
    sent = value.astype(SUM_TYPE)
    for step in range(1, size):
        pairs = [(i, i ^ step) for i in range(size)]
        total = total + lax.ppermute(sent, axis, pairs).astype(F32)
    return total


def write_piece(scaled, packed, up_ref, pieces_ref, piece):
    width = pieces_ref.shape[2]
    lanes = pl.ds(piece * width, width)
    sums = jnp.dot(scaled, up_ref[:, lanes], preferred_element_type=F32)
    place = member_order(pieces_ref.shape[0]).index(piece)
    pieces_ref[place, : scaled.shape[0], :] = sums.astype(BF16)
    pieces_ref[place, scaled.shape[0] :, :] = packed


def squares_row(h32):
    lanes = h32.shape[1]
    square = h32 * h32
    sums = jnp.sum(jnp.transpose(square), axis=0, keepdims=True)
    high = sums.astype(BF16).astype(F32)
    row = lax.broadcasted_iota(jnp.int32, (PAD, sums.shape[1]), 0)
    packed = jnp.where(row == 0, high, jnp.where(row == 1, sums - high, 0.0))
    rest = jnp.zeros((PAD, lanes - sums.shape[1]), F32)
    return jnp.concatenate([packed, rest], axis=1).astype(BF16)


def first_up_body(
    h_hbm, gain_hbm, up_hbm, pieces_hbm, h_ref, gain_ref, up_ref, pieces_ref, small_sems, in_sems, out_sems
):
    chunks = in_sems.shape[0]
    width = up_ref.shape[1] // chunks
    per_chunk = pieces_ref.shape[0] // chunks
    order = member_order(pieces_ref.shape[0])
    small = [
        pltpu.make_async_copy(h_hbm, h_ref, small_sems.at[0]),
        pltpu.make_async_copy(gain_hbm, gain_ref, small_sems.at[1]),
    ]
    arriving = [
        pltpu.make_async_copy(
            up_hbm.at[:, pl.ds(i * width, width)], up_ref.at[:, pl.ds(i * width, width)], in_sems.at[i]
        )
        for i in range(chunks)
    ]
    leaving = [
        pltpu.make_async_copy(
            pieces_ref.at[order.index(piece)], pieces_hbm.at[order.index(piece)], out_sems.at[piece]
        )
        for piece in range(len(order))
    ]
    for copy in small + arriving:
        copy.start()
    if STAGGER_NS:

        @pl.when(lax.axis_index("dp") == STAGGER_CORE)
        def _():
            pl.delay(STAGGER_NS)

    for copy in small:
        copy.wait()
    h32 = h_ref[...].astype(F32)
    scaled = (h32 * gain_ref[...]).astype(BF16)
    packed = squares_row(h32)
    for i in range(chunks):
        arriving[i].wait()
        for piece in range(i * per_chunk, (i + 1) * per_chunk):
            write_piece(scaled, packed, up_ref, pieces_ref, piece)
            leaving[piece].start()
    for copy in leaving:
        copy.wait()


def up_body(h_ref, gain_ref, up_ref, pieces_ref):
    h32 = h_ref[...].astype(F32)
    scaled = (h32 * gain_ref[:1]).astype(BF16)
    packed = squares_row(h32)
    for piece in range(pieces_ref.shape[0]):
        write_piece(scaled, packed, up_ref, pieces_ref, piece)


def up_shape(h, w_up):
    ra = lax.axis_size("ra")
    return jax.ShapeDtypeStruct((ra, h.shape[0] + PAD, w_up.shape[1] // ra), BF16)


def up_costs(h, w_up):
    return pl.CostEstimate(
        flops=2 * h.size * w_up.shape[1], bytes_accessed=UP_COST, transcendentals=0
    )


def first_up(h, gain, w_up):
    chunks = CHUNKS
    pieces = up_shape(h, w_up)
    hbm = pl.BlockSpec(memory_space=pl.ANY)
    return pl.pallas_call(
        first_up_body,
        out_shape=pieces,
        in_specs=[hbm] * 3,
        out_specs=hbm,
        scratch_shapes=[
            pltpu.VMEM(h.shape, h.dtype),
            pltpu.VMEM(gain.shape, gain.dtype),
            pltpu.VMEM(w_up.shape, w_up.dtype),
            pltpu.VMEM(pieces.shape, pieces.dtype),
            pltpu.SemaphoreType.DMA((2,)),
            pltpu.SemaphoreType.DMA((chunks,)),
            pltpu.SemaphoreType.DMA(pieces.shape[:1]),
        ],
        compiler_params=pltpu.CompilerParams(vmem_limit_bytes=66_000_000),
        cost_estimate=up_costs(h, w_up),
        name="first_up",
    )(h, gain, w_up)


def second_up(h, gain, w_up):
    return pl.pallas_call(
        up_body,
        out_shape=up_shape(h, w_up),
        compiler_params=pltpu.CompilerParams(vmem_limit_bytes=8 * 1024 * 1024),
        cost_estimate=up_costs(h, w_up),
        name="second_up",
    )(h, gain, w_up)


def down_body(everyone_ref, down_ref, out_ref):
    rows, lanes = out_ref.shape[0], everyone_ref.shape[2]
    order = member_order(everyone_ref.shape[0])
    total = jnp.zeros(out_ref.shape, F32)
    for block in range(0, len(order), 2):
        pair = [everyone_ref[order.index(block + k), :rows, :] for k in range(2)]
        weights = down_ref[pl.ds(block * lanes, 2 * lanes), :]
        total = total + jnp.dot(
            jnp.concatenate(pair, axis=1), weights, preferred_element_type=F32
        )
    out_ref[...] = total


def down_sums(everyone, w_down, rows):
    return pl.pallas_call(
        down_body,
        out_shape=jax.ShapeDtypeStruct((rows, w_down.shape[1]), F32),
        compiler_params=pltpu.CompilerParams(vmem_limit_bytes=8 * 1024 * 1024),
        cost_estimate=pl.CostEstimate(
            flops=2 * rows * w_down.size, bytes_accessed=UP_COST, transcendentals=0
        ),
        name="down_sums",
    )(everyone, w_down)


def branch_of(pieces, w_down, beside):
    ra, rows, lanes = pieces.shape
    rows -= PAD
    arrived, beside = lax.optimization_barrier((exchange(pieces), beside))
    shared = arrived[:, :rows].astype(F32).sum(axis=0)
    hidden_share = jnp.square(jax.nn.relu(shared)).astype(BF16)
    squares = arrived[:, rows : rows + 2, :rows].astype(F32).sum(axis=(0, 1))
    hidden_share, squares = lax.optimization_barrier((hidden_share, squares))
    everyone = sent_to_all(hidden_share)
    mean_sq = squares / (ra * w_down.shape[1])
    down = down_sums(everyone, w_down, rows)
    return summed_over(down, "cb") / (mean_sq + EPS)[:, None], beside


def local(tokens, gain_first, up_first, down_first, gain_second, up_second, down_second, gain_last):
    pieces = first_up(tokens, gain_first[None, :], up_first)
    pieces, tokens, gain_second, gain_last = lax.optimization_barrier(
        (pieces, tokens, gain_second, gain_last)
    )
    start = tokens.astype(F32)
    gains = lax.optimization_barrier(
        tuple(jnp.broadcast_to(gain, (*tokens.shape[:1], *gain.shape)) for gain in (gain_second, gain_last))
    )
    branch, gains = branch_of(pieces, down_first, gains)
    first = (0.5 * start + branch).astype(BF16)
    pieces = second_up(first, gains[0], up_second)
    branch, gains = branch_of(pieces, down_second, gains)
    second = (0.5 * first.astype(F32) + branch).astype(BF16)
    second32 = second.astype(F32)
    squares = sent_to_all(jnp.sum(second32 * second32, axis=1), LAST_LEAD_EIGHTHS).sum(axis=0)
    inverse = lax.rsqrt(squares / (lax.axis_size("ra") * second.shape[1]) + EPS)
    return (second32 * inverse[:, None] * gains[1]).astype(BF16)


def solution(mesh):
    return jax.shard_map(
        local,
        mesh=mesh,
        in_specs=(
            P(("grp", "dp"), "ra"),
            P("ra"),
            P("ra", "cb"),
            P("cb", "ra"),
            P("ra"),
            P("ra", "cb"),
            P("cb", "ra"),
            P("ra"),
        ),
        out_specs=P(("grp", "dp"), "ra"),
        check_vma=False,
    )
```

```python
import jax
import jax.numpy as jnp
from jax import lax
from jax.experimental import pallas as pl
from jax.experimental.pallas import tpu as pltpu
from jax.sharding import PartitionSpec as P

EPS = 1e-06
F32 = jnp.float32
BF16 = jnp.bfloat16
STAGGER_NS = 13300
STAGGER_CORE = 1
LEAD_EIGHTHS = 7
LAST_LEAD_EIGHTHS = 4
SUM_TYPE = BF16
UP_COST = 2 << 20
PAD = 8
CHUNKS = 1


def member_order(size, eighths=None):
    lead = size * (LEAD_EIGHTHS if eighths is None else eighths) // 8
    return [(lead + i) % size for i in range(size)]


def exchange(pieces, eighths=None):
    order = member_order(lax.axis_size("ra"), eighths)
    return lax.all_to_all(
        pieces, "ra", split_axis=0, concat_axis=0, tiled=True, axis_index_groups=[order]
    )


def sent_to_all(shard, eighths=None):
    return exchange(jnp.broadcast_to(shard, (lax.axis_size("ra"), *shard.shape)), eighths)


def summed_over(value, axis):
    size = lax.axis_size(axis)
    total = value
    sent = value.astype(SUM_TYPE)
    for step in range(1, size):
        pairs = [(i, i ^ step) for i in range(size)]
        total = total + lax.ppermute(sent, axis, pairs).astype(F32)
    return total


def write_piece(scaled, packed, up_ref, pieces_ref, piece):
    width = pieces_ref.shape[2]
    lanes = pl.ds(piece * width, width)
    sums = jnp.dot(scaled, up_ref[:, lanes], preferred_element_type=F32)
    place = member_order(pieces_ref.shape[0]).index(piece)
    pieces_ref[place, : scaled.shape[0], :] = sums.astype(BF16)
    pieces_ref[place, scaled.shape[0] :, :] = packed


def squares_row(h32):
    lanes = h32.shape[1]
    square = h32 * h32
    sums = jnp.sum(jnp.transpose(square), axis=0, keepdims=True)
    high = sums.astype(BF16).astype(F32)
    row = lax.broadcasted_iota(jnp.int32, (PAD, sums.shape[1]), 0)
    packed = jnp.where(row == 0, high, jnp.where(row == 1, sums - high, 0.0))
    rest = jnp.zeros((PAD, lanes - sums.shape[1]), F32)
    return jnp.concatenate([packed, rest], axis=1).astype(BF16)


def first_up_body(
    h_hbm, gain_hbm, up_hbm, pieces_hbm, h_ref, gain_ref, up_ref, pieces_ref, small_sems, in_sems, out_sems
):
    chunks = in_sems.shape[0]
    width = up_ref.shape[1] // chunks
    per_chunk = pieces_ref.shape[0] // chunks
    order = member_order(pieces_ref.shape[0])
    small = [
        pltpu.make_async_copy(h_hbm, h_ref, small_sems.at[0]),
        pltpu.make_async_copy(gain_hbm, gain_ref, small_sems.at[1]),
    ]
    arriving = [
        pltpu.make_async_copy(
            up_hbm.at[:, pl.ds(i * width, width)], up_ref.at[:, pl.ds(i * width, width)], in_sems.at[i]
        )
        for i in range(chunks)
    ]
    leaving = [
        pltpu.make_async_copy(
            pieces_ref.at[order.index(piece)], pieces_hbm.at[order.index(piece)], out_sems.at[piece]
        )
        for piece in range(len(order))
    ]
    for copy in small + arriving:
        copy.start()
    if STAGGER_NS:

        @pl.when(lax.axis_index("dp") == STAGGER_CORE)
        def _():
            pl.delay(STAGGER_NS)

    for copy in small:
        copy.wait()
    h32 = h_ref[...].astype(F32)
    scaled = (h32 * gain_ref[...]).astype(BF16)
    packed = squares_row(h32)
    for i in range(chunks):
        arriving[i].wait()
        for piece in range(i * per_chunk, (i + 1) * per_chunk):
            write_piece(scaled, packed, up_ref, pieces_ref, piece)
            leaving[piece].start()
    for copy in leaving:
        copy.wait()


def up_body(h_ref, gain_ref, up_ref, pieces_ref):
    h32 = h_ref[...].astype(F32)
    scaled = (h32 * gain_ref[:1]).astype(BF16)
    packed = squares_row(h32)
    for piece in range(pieces_ref.shape[0]):
        write_piece(scaled, packed, up_ref, pieces_ref, piece)


def up_shape(h, w_up):
    ra = lax.axis_size("ra")
    return jax.ShapeDtypeStruct((ra, h.shape[0] + PAD, w_up.shape[1] // ra), BF16)


def up_costs(h, w_up):
    return pl.CostEstimate(
        flops=2 * h.size * w_up.shape[1], bytes_accessed=UP_COST, transcendentals=0
    )


def first_up(h, gain, w_up):
    chunks = CHUNKS
    pieces = up_shape(h, w_up)
    hbm = pl.BlockSpec(memory_space=pl.ANY)
    return pl.pallas_call(
        first_up_body,
        out_shape=pieces,
        in_specs=[hbm] * 3,
        out_specs=hbm,
        scratch_shapes=[
            pltpu.VMEM(h.shape, h.dtype),
            pltpu.VMEM(gain.shape, gain.dtype),
            pltpu.VMEM(w_up.shape, w_up.dtype),
            pltpu.VMEM(pieces.shape, pieces.dtype),
            pltpu.SemaphoreType.DMA((2,)),
            pltpu.SemaphoreType.DMA((chunks,)),
            pltpu.SemaphoreType.DMA(pieces.shape[:1]),
        ],
        compiler_params=pltpu.CompilerParams(vmem_limit_bytes=66_000_000),
        cost_estimate=up_costs(h, w_up),
        name="first_up",
    )(h, gain, w_up)


def second_up(h, gain, w_up):
    return pl.pallas_call(
        up_body,
        out_shape=up_shape(h, w_up),
        compiler_params=pltpu.CompilerParams(vmem_limit_bytes=8 * 1024 * 1024),
        cost_estimate=up_costs(h, w_up),
        name="second_up",
    )(h, gain, w_up)


def down_body(everyone_ref, down_ref, out_ref):
    rows, lanes = out_ref.shape[0], everyone_ref.shape[2]
    order = member_order(everyone_ref.shape[0])
    total = jnp.zeros(out_ref.shape, F32)
    for block in range(0, len(order), 2):
        pair = [everyone_ref[order.index(block + k), :rows, :] for k in range(2)]
        weights = down_ref[pl.ds(block * lanes, 2 * lanes), :]
        total = total + jnp.dot(
            jnp.concatenate(pair, axis=1), weights, preferred_element_type=F32
        )
    out_ref[...] = total


def down_sums(everyone, w_down, rows):
    return pl.pallas_call(
        down_body,
        out_shape=jax.ShapeDtypeStruct((rows, w_down.shape[1]), F32),
        compiler_params=pltpu.CompilerParams(vmem_limit_bytes=8 * 1024 * 1024),
        cost_estimate=pl.CostEstimate(
            flops=2 * rows * w_down.size, bytes_accessed=UP_COST, transcendentals=0
        ),
        name="down_sums",
    )(everyone, w_down)


def branch_of(pieces, w_down, beside):
    ra, rows, lanes = pieces.shape
    rows -= PAD
    arrived, beside = lax.optimization_barrier((exchange(pieces), beside))
    shared = arrived[:, :rows].astype(F32).sum(axis=0)
    hidden_share = jnp.square(jax.nn.relu(shared)).astype(BF16)
    squares = arrived[:, rows : rows + 2, :rows].astype(F32).sum(axis=(0, 1))
    hidden_share, squares = lax.optimization_barrier((hidden_share, squares))
    everyone = sent_to_all(hidden_share)
    mean_sq = squares / (ra * w_down.shape[1])
    down = down_sums(everyone, w_down, rows)
    return summed_over(down, "cb") / (mean_sq + EPS)[:, None], beside


def local(tokens, gain_first, up_first, down_first, gain_second, up_second, down_second, gain_last):
    pieces = first_up(tokens, gain_first[None, :], up_first)
    pieces, tokens, gain_second, gain_last = lax.optimization_barrier(
        (pieces, tokens, gain_second, gain_last)
    )
    start = tokens.astype(F32)
    gains = lax.optimization_barrier(
        tuple(jnp.broadcast_to(gain, (*tokens.shape[:1], *gain.shape)) for gain in (gain_second, gain_last))
    )
    branch, gains = branch_of(pieces, down_first, gains)
    first = (0.5 * start + branch).astype(BF16)
    pieces = second_up(first, gains[0], up_second)
    branch, gains = branch_of(pieces, down_second, gains)
    second = (0.5 * first.astype(F32) + branch).astype(BF16)
    second32 = second.astype(F32)
    squares = sent_to_all(jnp.sum(second32 * second32, axis=1), LAST_LEAD_EIGHTHS).sum(axis=0)
    inverse = lax.rsqrt(squares / (lax.axis_size("ra") * second.shape[1]) + EPS)
    return (second32 * inverse[:, None] * gains[1]).astype(BF16)


def solution(mesh):
    return jax.shard_map(
        local,
        mesh=mesh,
        in_specs=(
            P(("grp", "dp"), "ra"),
            P("ra"),
            P("ra", "cb"),
            P("cb", "ra"),
            P("ra"),
            P("ra", "cb"),
            P("cb", "ra"),
            P("ra"),
        ),
        out_specs=P(("grp", "dp"), "ra"),
        check_vma=False,
    )
```

```python
import jax
import jax.numpy as jnp
from jax import lax
from jax.experimental import pallas as pl
from jax.experimental.pallas import tpu as pltpu
from jax.sharding import PartitionSpec as P

EPS = 1e-06
F32 = jnp.float32
BF16 = jnp.bfloat16
STAGGER_NS = 13300
STAGGER_CORE = 1
LEAD_EIGHTHS = 7
LAST_LEAD_EIGHTHS = 5
SUM_TYPE = BF16
UP_COST = 2 << 20
PAD = 8
CHUNKS = 2


def member_order(size, eighths=None):
    lead = size * (LEAD_EIGHTHS if eighths is None else eighths) // 8
    return [(lead + i) % size for i in range(size)]


def exchange(pieces, eighths=None):
    order = member_order(lax.axis_size("ra"), eighths)
    return lax.all_to_all(
        pieces, "ra", split_axis=0, concat_axis=0, tiled=True, axis_index_groups=[order]
    )


def sent_to_all(shard, eighths=None):
    return exchange(jnp.broadcast_to(shard, (lax.axis_size("ra"), *shard.shape)), eighths)


def summed_over(value, axis):
    size = lax.axis_size(axis)
    total = value
    sent = value.astype(SUM_TYPE)
    for step in range(1, size):
        pairs = [(i, i ^ step) for i in range(size)]
        total = total + lax.ppermute(sent, axis, pairs).astype(F32)
    return total


def write_piece(scaled, packed, up_ref, pieces_ref, piece):
    width = pieces_ref.shape[2]
    lanes = pl.ds(piece * width, width)
    sums = jnp.dot(scaled, up_ref[:, lanes], preferred_element_type=F32)
    place = member_order(pieces_ref.shape[0]).index(piece)
    pieces_ref[place, : scaled.shape[0], :] = sums.astype(BF16)
    pieces_ref[place, scaled.shape[0] :, :] = packed


def squares_row(h32):
    lanes = h32.shape[1]
    square = h32 * h32
    sums = jnp.sum(jnp.transpose(square), axis=0, keepdims=True)
    high = sums.astype(BF16).astype(F32)
    row = lax.broadcasted_iota(jnp.int32, (PAD, sums.shape[1]), 0)
    packed = jnp.where(row == 0, high, jnp.where(row == 1, sums - high, 0.0))
    rest = jnp.zeros((PAD, lanes - sums.shape[1]), F32)
    return jnp.concatenate([packed, rest], axis=1).astype(BF16)


def first_up_body(
    h_hbm, gain_hbm, up_hbm, pieces_hbm, h_ref, gain_ref, up_ref, pieces_ref, small_sems, in_sems, out_sems
):
    chunks = in_sems.shape[0]
    width = up_ref.shape[1] // chunks
    per_chunk = pieces_ref.shape[0] // chunks
    order = member_order(pieces_ref.shape[0])
    small = [
        pltpu.make_async_copy(h_hbm, h_ref, small_sems.at[0]),
        pltpu.make_async_copy(gain_hbm, gain_ref, small_sems.at[1]),
    ]
    arriving = [
        pltpu.make_async_copy(
            up_hbm.at[:, pl.ds(i * width, width)], up_ref.at[:, pl.ds(i * width, width)], in_sems.at[i]
        )
        for i in range(chunks)
    ]
    leaving = [
        pltpu.make_async_copy(
            pieces_ref.at[order.index(piece)], pieces_hbm.at[order.index(piece)], out_sems.at[piece]
        )
        for piece in range(len(order))
    ]
    for copy in small + arriving:
        copy.start()
    if STAGGER_NS:

        @pl.when(lax.axis_index("dp") == STAGGER_CORE)
        def _():
            pl.delay(STAGGER_NS)

    for copy in small:
        copy.wait()
    h32 = h_ref[...].astype(F32)
    scaled = (h32 * gain_ref[...]).astype(BF16)
    packed = squares_row(h32)
    for i in range(chunks):
        arriving[i].wait()
        for piece in range(i * per_chunk, (i + 1) * per_chunk):
            write_piece(scaled, packed, up_ref, pieces_ref, piece)
            leaving[piece].start()
    for copy in leaving:
        copy.wait()


def up_body(h_ref, gain_ref, up_ref, pieces_ref):
    h32 = h_ref[...].astype(F32)
    scaled = (h32 * gain_ref[:1]).astype(BF16)
    packed = squares_row(h32)
    for piece in range(pieces_ref.shape[0]):
        write_piece(scaled, packed, up_ref, pieces_ref, piece)


def up_shape(h, w_up):
    ra = lax.axis_size("ra")
    return jax.ShapeDtypeStruct((ra, h.shape[0] + PAD, w_up.shape[1] // ra), BF16)


def up_costs(h, w_up):
    return pl.CostEstimate(
        flops=2 * h.size * w_up.shape[1], bytes_accessed=UP_COST, transcendentals=0
    )


def first_up(h, gain, w_up):
    chunks = CHUNKS
    pieces = up_shape(h, w_up)
    hbm = pl.BlockSpec(memory_space=pl.ANY)
    return pl.pallas_call(
        first_up_body,
        out_shape=pieces,
        in_specs=[hbm] * 3,
        out_specs=hbm,
        scratch_shapes=[
            pltpu.VMEM(h.shape, h.dtype),
            pltpu.VMEM(gain.shape, gain.dtype),
            pltpu.VMEM(w_up.shape, w_up.dtype),
            pltpu.VMEM(pieces.shape, pieces.dtype),
            pltpu.SemaphoreType.DMA((2,)),
            pltpu.SemaphoreType.DMA((chunks,)),
            pltpu.SemaphoreType.DMA(pieces.shape[:1]),
        ],
        compiler_params=pltpu.CompilerParams(vmem_limit_bytes=66_000_000),
        cost_estimate=up_costs(h, w_up),
        name="first_up",
    )(h, gain, w_up)


def second_up(h, gain, w_up):
    return pl.pallas_call(
        up_body,
        out_shape=up_shape(h, w_up),
        compiler_params=pltpu.CompilerParams(vmem_limit_bytes=8 * 1024 * 1024),
        cost_estimate=up_costs(h, w_up),
        name="second_up",
    )(h, gain, w_up)


def down_body(everyone_ref, down_ref, out_ref):
    rows, lanes = out_ref.shape[0], everyone_ref.shape[2]
    order = member_order(everyone_ref.shape[0])
    total = jnp.zeros(out_ref.shape, F32)
    for block in range(0, len(order), 2):
        pair = [everyone_ref[order.index(block + k), :rows, :] for k in range(2)]
        weights = down_ref[pl.ds(block * lanes, 2 * lanes), :]
        total = total + jnp.dot(
            jnp.concatenate(pair, axis=1), weights, preferred_element_type=F32
        )
    out_ref[...] = total


def down_sums(everyone, w_down, rows):
    return pl.pallas_call(
        down_body,
        out_shape=jax.ShapeDtypeStruct((rows, w_down.shape[1]), F32),
        compiler_params=pltpu.CompilerParams(vmem_limit_bytes=8 * 1024 * 1024),
        cost_estimate=pl.CostEstimate(
            flops=2 * rows * w_down.size, bytes_accessed=UP_COST, transcendentals=0
        ),
        name="down_sums",
    )(everyone, w_down)


def branch_of(pieces, w_down, beside):
    ra, rows, lanes = pieces.shape
    rows -= PAD
    arrived, beside = lax.optimization_barrier((exchange(pieces), beside))
    shared = arrived[:, :rows].astype(F32).sum(axis=0)
    hidden_share = jnp.square(jax.nn.relu(shared)).astype(BF16)
    squares = arrived[:, rows : rows + 2, :rows].astype(F32).sum(axis=(0, 1))
    hidden_share, squares = lax.optimization_barrier((hidden_share, squares))
    everyone = sent_to_all(hidden_share)
    mean_sq = squares / (ra * w_down.shape[1])
    down = down_sums(everyone, w_down, rows)
    return summed_over(down, "cb") / (mean_sq + EPS)[:, None], beside


def local(tokens, gain_first, up_first, down_first, gain_second, up_second, down_second, gain_last):
    pieces = first_up(tokens, gain_first[None, :], up_first)
    pieces, tokens, gain_second, gain_last = lax.optimization_barrier(
        (pieces, tokens, gain_second, gain_last)
    )
    start = tokens.astype(F32)
    gains = lax.optimization_barrier(
        tuple(jnp.broadcast_to(gain, (*tokens.shape[:1], *gain.shape)) for gain in (gain_second, gain_last))
    )
    branch, gains = branch_of(pieces, down_first, gains)
    first = (0.5 * start + branch).astype(BF16)
    pieces = second_up(first, gains[0], up_second)
    branch, gains = branch_of(pieces, down_second, gains)
    second = (0.5 * first.astype(F32) + branch).astype(BF16)
    second32 = second.astype(F32)
    squares = sent_to_all(jnp.sum(second32 * second32, axis=1), LAST_LEAD_EIGHTHS).sum(axis=0)
    inverse = lax.rsqrt(squares / (lax.axis_size("ra") * second.shape[1]) + EPS)
    return (second32 * inverse[:, None] * gains[1]).astype(BF16)


def solution(mesh):
    return jax.shard_map(
        local,
        mesh=mesh,
        in_specs=(
            P(("grp", "dp"), "ra"),
            P("ra"),
            P("ra", "cb"),
            P("cb", "ra"),
            P("ra"),
            P("ra", "cb"),
            P("cb", "ra"),
            P("ra"),
        ),
        out_specs=P(("grp", "dp"), "ra"),
        check_vma=False,
    )
```
